32 devices in a mesh: fs: 4 (over z), tp: 8 (over y, x, core).
Axes of the slice: x: 2, y: 2, z: 4, core: 2. Of those that a mesh axis runs over, the one named last changes fastest.
Arguments:
- tokens: bfloat16 [1024, 2048], P('fs', 'tp'), may hold values from -6 to 6
- norm_gain: float32 [2048], P('tp'), may hold values from 0.1 to 1.9
- gate_master: float32 [8, 3584, 2048], P(None, 'fs', 'tp'), may hold values from -0.125 to 0.125
- up_master: float32 [8, 3584, 2048], P(None, 'fs', 'tp'), may hold values from -0.125 to 0.125
- down_master: float32 [8, 3584, 2048], P(None, 'fs', 'tp'), may hold values from -0.0625 to 0.0625
- routes: int32 [1024, 2], P('fs'), may hold values from 0 to 3, all different within a row; in each aligned block of 256 rows (0 to 255, 256 to 511, ...) at most 128 rows name the same one
- route_logits: float32 [1024, 2], P('fs'), may hold values from -8 to 8
Outputs:
- gate_serve: bfloat16 [8, 3584, 2048], P('tp', 'fs')
- up_serve: bfloat16 [8, 3584, 2048], P('tp', 'fs')
- down_serve: bfloat16 [8, 3584, 2048], P('tp', 'fs')
- mixed_tokens: bfloat16 [1024, 2048], P('fs', 'tp')
The draws below stay inside these ranges and needn't reach their ends.
Inputs may be any that keep to these rules, and one draw needn't show every extreme that they name: `routes`: each row names 2 different experts; in every aligned block of 256 rows each expert is named by exactly 128 rows.
All inputs are finite; a program needn't handle non-finite values.
Results may differ from the reference program's by a relative error of at most 0.024.
Values may be sent and summed in bfloat16 or wider, within the bound.
A program may use at most 128 MiB of HBM per device.

```python
import math
import jax
import jax.numpy as jnp
import numpy as np
from jax import lax

D = 2048
FF = 7168
TOP = 2
TOK_DEV = 256
EXPERTS = 4
SLABS = 8
FF_SLAB = 3584
TOKENS = 1024
CAP = 128
N_FS = 4


def block_levels(key, extent, pieces, low, top_value):
    def one(position, shards_of):
        steps = jax.random.uniform(jax.random.fold_in(jax.random.fold_in(key, 6), position), (shards_of,), jnp.float32, low / len(pieces), top_value / len(pieces))
        return jnp.repeat(jnp.exp(steps), extent[position] // shards_of).reshape((-1,) + (1,) * (len(extent) - position - 1))

    factor_of = one(*pieces[0])
    for cut in pieces[1:]:
        factor_of = factor_of * one(*cut)
    return factor_of


def assign_block(own_key, own, number, rows, number_of, top, bound, lean):
    order = jax.random.permutation(own_key, number_of)
    crowded, common = portions_of(number_of, rows * top, bound, lean, True), portions_of(number_of, rows * top, bound, lean, False)
    places = jnp.arange(number_of)

    def named(sizes, offset_by):
        used = int((sizes > 0).sum())
        fixed = max(1, used // 4)
        shifted = fixed + (places - fixed + offset_by * (used - fixed)) % max(1, number_of - fixed)
        return jnp.zeros((number_of,), jnp.int32).at[order[jnp.where(places < fixed, places, shifted)]].set(jnp.asarray(sizes, jnp.int32))

    sizes = jnp.where(number % 4 == 0, named(crowded, number // 4), named(common, number - number // 4 - 1))
    mixed = jax.random.permutation(jax.random.fold_in(own, 3), number_of)
    giver, sink = mixed[0:number_of // 2 * 2:2], mixed[1:number_of // 2 * 2:2]
    margin = jnp.minimum(sizes[giver] - 1, bound - sizes[sink]) // 2
    margin = jnp.where((giver == order[0]) | (sink == order[0]) | (sizes[sink] == 0), 0, jnp.maximum(margin, 0))
    shifted = jax.random.randint(jax.random.fold_in(own, 4), (number_of // 2,), 0, 1 << 20) % (margin + 1)
    sizes = sizes.at[giver].add(-shifted).at[sink].add(shifted)
    items = jnp.searchsorted(jnp.cumsum(sizes), jnp.arange(rows * top), side="right").astype(jnp.int32)
    grid = items.reshape(top, rows).T
    grid = grid[jax.random.permutation(jax.random.fold_in(own, 1), rows)]
    offset_by = jax.random.randint(jax.random.fold_in(own, 2), (rows, 1), 0, top)
    return jnp.take_along_axis(grid, (jnp.arange(top)[None, :] + offset_by) % top, axis=1)


def portions_of(number_of, total, limit, slope, full):
    weights = [(1 << 20) // math.isqrt(standing ** slope) + 1 for standing in range(1, number_of + 1)]
    largest = limit if full else min(limit, max(-(-total // number_of), total * weights[0] // sum(weights)))
    least = 1 if total - largest >= number_of - 1 else 0
    counts, spare = [largest] + [least] * (number_of - 1), total - largest - least * (number_of - 1)
    while spare > 0:
        candidates = [i for i in range(1, number_of) if counts[i] < largest] or [i for i in range(1, number_of) if counts[i] < limit]
        pool, left = sum([weights[i] for i in candidates]), spare
        for i in candidates:
            addition = min(limit - counts[i], max(1, left * weights[i] // pool), spare)
            counts[i] = counts[i] + addition
            spare = spare - addition
    return np.array(counts)


def normal_values(key, shape, width, limit, split=(), kind=jnp.bfloat16):
    drawn = width * jax.random.normal(key, shape, jnp.float32)
    if split:
        drawn = drawn * block_levels(key, shape, split, -0.22, 0.18)
    return jnp.clip(drawn, -limit, limit).astype(kind)


def setup_inputs(seed: int = 0) -> dict:
    seeds = jax.random.split(jax.random.key(seed), 8)
    tokens = normal_values(seeds[0], (TOKENS, D), 1.0, 6.0, ((0, 4), (1, 8)))
    norm_gain = jnp.clip(1.0 + 0.18 * jax.random.normal(seeds[1], (D,), jnp.float32), 0.1, 1.9)
    gate_master = normal_values(seeds[2], (SLABS, FF_SLAB, D), D ** -0.5, 0.125, ((1, 4), (2, 8)), jnp.float32)
    up_master = normal_values(seeds[3], (SLABS, FF_SLAB, D), D ** -0.5, 0.125, ((1, 4), (2, 8)), jnp.float32)
    down_master = normal_values(seeds[4], (SLABS, FF_SLAB, D), FF ** -0.5, 0.0625, ((1, 4), (2, 8)), jnp.float32)
    routes_keys = jax.random.split(jax.random.fold_in(seeds[5], 1), TOKENS // TOK_DEV)
    routes_turns = jax.random.permutation(jax.random.fold_in(seeds[5], 3), TOKENS // TOK_DEV)
    routes = jax.vmap(lambda own, number: assign_block(jax.random.fold_in(seeds[5], 2), own, number, TOK_DEV, EXPERTS, TOP, CAP, 0))(routes_keys, routes_turns).reshape((TOKENS, TOP))
    route_logits = normal_values(seeds[6], (TOKENS, TOP), 2.0, 8.0, ((0, 4),), jnp.float32)
    return dict(tokens=tokens, norm_gain=norm_gain, gate_master=gate_master, up_master=up_master, down_master=down_master, routes=routes, route_logits=route_logits)


epsilon = 1e-05

def reference(tokens, norm_gain, gate_master, up_master, down_master, routes, route_logits):
    gain_row = norm_gain[None, None, :]
    gate_serve = (gate_master * gain_row).astype(jnp.bfloat16)
    up_serve = (up_master * gain_row).astype(jnp.bfloat16)
    down_serve = down_master.astype(jnp.bfloat16)
    widened = tokens.astype(jnp.float32)
    row_scale = lax.rsqrt(lax.optimization_barrier(jnp.mean(widened * widened, axis=-1, keepdims=True)) + epsilon)
    normed = (widened * row_scale).astype(jnp.bfloat16)
    first_prob = jax.nn.sigmoid(route_logits[:, 0] - route_logits[:, 1])
    choice_prob = jnp.stack([first_prob, 1.0 - first_prob], axis=1)
    row_total = N_FS * CAP
    block_rows = FF_SLAB // N_FS

    def one_expert(expert_id):
        matches = routes == expert_id
        is_member = jnp.any(matches, axis=1)
        weight = lax.optimization_barrier(jnp.sum(jnp.where(matches, choice_prob, 0.0), axis=1))
        row_index = jnp.nonzero(is_member, size=row_total)[0].astype(jnp.int32)
        picked = normed[row_index]
        block_parts = jnp.zeros((N_FS, row_total, D), jnp.float32)
        for half_index in range(2):
            slab_id = 2 * expert_id + half_index
            gate_slab = lax.dynamic_index_in_dim(gate_serve, slab_id, 0, keepdims=False)
            up_slab = lax.dynamic_index_in_dim(up_serve, slab_id, 0, keepdims=False)
            down_slab = lax.dynamic_index_in_dim(down_serve, slab_id, 0, keepdims=False)
            gate_pre = jnp.dot(picked, gate_slab.T, preferred_element_type=jnp.float32)
            up_pre = jnp.dot(picked, up_slab.T, preferred_element_type=jnp.float32)
            hidden = (jax.nn.silu(gate_pre) * up_pre).astype(jnp.bfloat16)
            block_parts = block_parts + jnp.einsum('rfk,fkd->frd', hidden.reshape(row_total, N_FS, block_rows).astype(jnp.float32), down_slab.reshape(N_FS, block_rows, D).astype(jnp.float32))
        rounded = lax.optimization_barrier(block_parts.astype(jnp.bfloat16))
        expert_out = lax.optimization_barrier(jnp.sum(rounded.astype(jnp.float32), axis=0)).astype(jnp.bfloat16)
        return (row_index, weight[row_index][:, None] * expert_out.astype(jnp.float32))
    expert_ids = jnp.arange(EXPERTS, dtype=jnp.int32)
    all_index, all_terms = lax.map(one_expert, expert_ids)
    mixed = jnp.zeros((TOKENS, D), jnp.float32).at[all_index.reshape(-1)].add(all_terms.reshape(-1, D))
    return (gate_serve, up_serve, down_serve, mixed.astype(jnp.bfloat16))
```

```python
import functools

import jax
import jax.numpy as jnp
from jax import lax
from jax.experimental import pallas as pl
from jax.experimental.pallas import tpu as pltpu
from jax.sharding import PartitionSpec as P

epsilon = 1e-05
MESH = pl.DeviceIdType.MESH
NT = (((1,), (1,)), ((), ()))
NN = (((1,), (0,)), ((), ()))
TN = (((0,), (0,)), ((), ()))
SLOTS = 4
EARLY = 1


def dot(a, b, dims):
    return lax.dot_general(a, b, dims, preferred_element_type=jnp.float32)


def flipped(index, mask):
    result, bit = index, 1
    while bit <= mask:
        if mask & bit:
            result = result + bit * (1 - 2 * ((index // bit) % 2))
        bit *= 2
    return result


def kernel(
    nf, nt, tok_hbm, gain_hbm, gate_ref, up_ref, down_ref, routes_hbm, logits_hbm,
    wgu, wd, ret, comb_hi, comb_lo,
    tok, gain_ref, routes_ref, logits_ref, stage, snd, sdn, pick, xin, xall, gate_pre, hid,
    ship, pin, psum, zin, fin,
    in_sem, stage_sem, w_send, w_recv, d_send, d_recv, x_send, x_recv, z_send, z_recv, p_send, p_recv,
    h_send, h_recv, s_send, s_recv, r_send, r_recv,
):
    f, me = lax.axis_index("fs"), lax.axis_index("tp")
    parity = me % 2
    partner = me + 1 - 2 * parity
    rows, cols = tok.shape
    block = gate_ref.shape[1]
    parts, cc = wd.shape[1], wd.shape[3]
    half = pick.shape[1]
    cap = 2 * half
    experts = nt // 2
    pairs = nt // 2
    masters = (gate_ref, up_ref, down_ref)
    corner = [c for c in range(pairs - 1, 0, -1) if c.bit_count() > 1]
    near = [1] if pairs > 1 else []
    later = [c for c in range(pairs - 1, 1, -1) if c not in corner]

    def both(chips):
        return [k for c in chips for k in (2 * c + 1, 2 * c)]

    order = both(corner + near + later) + [1, 0]
    last = both(near + later) + [1, 0] + both(corner)
    jobs = [(w, k) for w in range(2) for k in order] + [(2, k) for k in last]

    def load(i):
        w, k = jobs[i]
        return pltpu.make_async_copy(
            masters[w].at[flipped(me, k)], stage.at[i % SLOTS], stage_sem.at[i % SLOTS]
        )

    def remote(src, dst, send, recv, to_f, to_t):
        return pltpu.make_async_remote_copy(
            src_ref=src, dst_ref=dst, send_sem=send, recv_sem=recv,
            device_id=(to_f, to_t), device_id_type=MESH,
        )

    small = [
        pltpu.make_async_copy(a, b, in_sem.at[i])
        for i, (a, b) in enumerate(
            ((gain_hbm, gain_ref), (routes_hbm, routes_ref), (logits_hbm, logits_ref), (tok_hbm, tok))
        )
    ]
    load(0).start()
    for copy in small:
        copy.start()
    for i in range(1, SLOTS):
        load(i).start()
    barrier = pltpu.get_barrier_semaphore()
    for k in range(1, nt):
        pl.semaphore_signal(barrier, inc=1, device_id=(f, flipped(me, k)), device_id_type=MESH)

    @pl.loop(1, nf)
    def _(d):
        pl.semaphore_signal(barrier, inc=1, device_id=((f + d) % nf, me), device_id_type=MESH)

    step = 128 if block % 128 == 0 else block

    def weight_copy(w, k):
        return remote(
            snd.at[w, k - 1], wgu.at[w, me], w_send.at[w, k - 1], w_recv.at[w, k - 1], f, flipped(me, k)
        )

    def down_copy(k, p):
        return remote(
            sdn.at[k - 1, p], wd.at[me, p], d_send.at[k - 1, p], d_recv.at[k - 1, p], f, flipped(me, k)
        )

    def convert(i):
        w, k = jobs[i]
        slot = i % SLOTS
        load(i).wait()
        gain = gain_ref[...]

        @pl.loop(0, block // step)
        def _(c):
            at = pl.ds(pl.multiple_of(c * step, 16), step)
            value = stage[slot, at, :]
            if w < 2:
                value = (value * gain).astype(jnp.bfloat16)
                if k:
                    snd[w, k - 1, at, :] = value
                else:
                    wgu[w, me, at, :] = value
            else:
                value = value.astype(jnp.bfloat16)
                for p in range(parts):
                    piece = value[:, p * cc : (p + 1) * cc]
                    if k:
                        sdn[k - 1, p, at, :] = piece
                    else:
                        wd[me, p, at, :] = piece

        if i + SLOTS < len(jobs):
            load(i + SLOTS).start()

    def send(i):
        w, k = jobs[i]
        if not k or k // 2 in later:
            return
        if w < 2:
            weight_copy(w, k).start()
        elif k % 2 == 0:
            for p in range(parts):
                down_copy(k + 1, p).start()
                down_copy(k, p).start()
        elif k == 1:
            for p in range(parts):
                down_copy(k, p).start()

    def x_copy(k):
        to = flipped(me, k)
        return remote(pick.at[to], xin.at[me], x_send.at[k - 1], x_recv.at[k - 1], f, to)

    def route():
        for copy in small[1:]:
            copy.wait()
        r0, r1 = routes_ref[0:1, :], routes_ref[1:2, :]
        l0, l1 = logits_ref[0:1, :], logits_ref[1:2, :]
        p0 = 1.0 / (1.0 + jnp.exp(l1 - l0))
        p1 = 1.0 / (1.0 + jnp.exp(l0 - l1))
        padded = -(-experts // 8) * 8
        ids = lax.broadcasted_iota(jnp.int32, (padded, rows), 0)
        first = jnp.where(ids == r0, 1.0, 0.0)
        second = jnp.where(ids == r1, 1.0, 0.0)
        chosen = first + second
        weight = first * p0 + second * p1
        before = lax.broadcasted_iota(jnp.int32, (rows, rows), 0)
        after = lax.broadcasted_iota(jnp.int32, (rows, rows), 1)
        upto = jnp.where(before <= after, 1.0, 0.0).astype(jnp.bfloat16)
        position = dot(chosen.astype(jnp.bfloat16), upto, NN) - 1.0
        slots = lax.broadcasted_iota(jnp.int32, (cap, rows), 0).astype(jnp.float32)
        for e in range(experts):
            hit = jnp.where(slots == position[e : e + 1, :], 1.0, 0.0) * chosen[e : e + 1, :]
            placed = hit.astype(jnp.bfloat16)
            scaled = hit * weight[e : e + 1, :]
            high = scaled.astype(jnp.bfloat16)
            at = pl.ds(e * cap, cap)
            comb_hi[at, :] = high
            comb_lo[at, :] = (scaled - high.astype(jnp.float32)).astype(jnp.bfloat16)
            got = dot(placed, tok[...], NN).astype(jnp.bfloat16)
            pick[2 * e] = got[:half]
            pick[2 * e + 1] = got[half:]
        xin[me] = pick[me]
        for k in order[:-1]:
            x_copy(k).start()

    small[0].wait()
    for i in range(EARLY):
        convert(i)
    pl.semaphore_wait(barrier, nt - 1 + nf - 1)
    for i in range(EARLY):
        send(i)
    route()
    for i in range(EARLY, len(jobs)):
        convert(i)
        send(i)

    def release(w):
        for k in both(corner):
            weight_copy(w, k).wait_send()
        for k in both(later):
            weight_copy(w, k).start()

    release(0)

    for k in order[:-1]:
        x_copy(k).wait_recv()
    total = jnp.zeros((half, 1), jnp.float32)
    for s in range(nt):
        v = xin[s].astype(jnp.float32)
        total = total + jnp.sum(v * v, axis=-1, keepdims=True)
    scale = lax.rsqrt(total / (nt * cols) + epsilon)

    def rows_of(p, g):
        return pl.ds(pl.multiple_of((2 * g + p) * half, 16), half)

    mine = rows_of(parity, f)
    for s in range(nt):
        xall[s, mine, :] = (xin[s].astype(jnp.float32) * scale).astype(jnp.bfloat16)

    def z_copy(d):
        here = xall.at[:, mine, :]
        return remote(here, here, z_send.at[d], z_recv.at[d], (f + d) % nf, me)

    def p_copy(d):
        here = xall.at[:, rows_of(parity, (f + nf - d) % nf), :]
        return remote(here, here, p_send.at[d], p_recv.at[d], f, partner)

    p_copy(0).start()

    @pl.loop(1, nf)
    def _(d):
        z_copy(d).start()

    @pl.loop(1, nf)
    def _(d):
        here = xall.at[:, rows_of(parity, (f + nf - d) % nf), :]
        remote(here, here, z_send.at[d], z_recv.at[d], (f + d) % nf, me).wait_recv()
        p_copy(d).start()

    @pl.loop(0, nf)
    def _(d):
        here = xall.at[:, rows_of(1 - parity, (f + nf - d) % nf), :]
        remote(here, here, p_send.at[d], p_recv.at[d], f, partner).wait_recv()

    def arrived(w, k):
        if k:
            s = flipped(me, k)
            remote(
                snd.at[w, k - 1], wgu.at[w, s], w_send.at[w, k - 1], w_recv.at[w, k - 1], f, s
            ).wait_recv()

    def product(w, at):
        acc = dot(xall[0], wgu[w, 0, at, :], NT)
        for s in range(1, nt):
            acc = acc + dot(xall[s], wgu[w, s, at, :], NT)
        return acc

    def tile(c):
        return pl.ds(pl.multiple_of(c * step, 16), step)

    def lanes(c):
        return pl.ds(pl.multiple_of(c * step, 128), step) if block % 128 == 0 else slice(None)

    for k in order:
        arrived(0, k)

    @pl.loop(0, block // step)
    def _(c):
        gate_pre[:, lanes(c)] = product(0, tile(c))

    release(1)
    for c in later:
        for p in range(parts):
            down_copy(2 * c + 1, p).start()
            down_copy(2 * c, p).start()
    for k in order:
        arrived(1, k)

    @pl.loop(0, block // step)
    def _(c):
        gate = gate_pre[:, lanes(c)]
        hid[:, lanes(c)] = (gate / (1.0 + jnp.exp(-gate)) * product(1, tile(c))).astype(jnp.bfloat16)

    groups = [(0, p) for p in range(parts)]
    groups += [(c, p) for p in range(parts) for c in near + later]
    groups += [(c, p) for p in range(parts) for c in corner]

    def took(k, p):
        s = flipped(me, k)
        if k:
            remote(
                sdn.at[k - 1, p], wd.at[s, p], d_send.at[k - 1, p], d_recv.at[k - 1, p], f, s
            ).wait_recv()
        return dot(hid[...], wd[s, p], NN)

    def h_copy(c, p):
        return remote(ship.at[c, p], pin.at[c, p], h_send.at[c, p], h_recv.at[c, p], f, partner)

    def s_copy(c, p, d):
        to = (f + d) % nf
        return remote(psum.at[c, p, to], zin.at[c, p, d], s_send.at[c, p, d], s_recv.at[c, p, d], to, me)

    def r_copy(c, p):
        return remote(
            fin.at[c, p], ret.at[p, pl.ds(pl.multiple_of((me // 2) * cap, 16), cap), :],
            r_send.at[c, p], r_recv.at[c, p], f, flipped(me, 2 * c),
        )

    def stage_a(c, p):
        ship[c, p] = took(2 * c + 1, p).astype(jnp.bfloat16)
        h_copy(c, p).start()

    def stage_b(c, p):
        own = took(2 * c, p)
        h_copy(c, p).wait_recv()
        total = (own + pin[c, p].astype(jnp.float32)).astype(jnp.bfloat16)
        for j in range(nf):
            psum[c, p, j] = total[j * cap : (j + 1) * cap]

        @pl.loop(1, nf)
        def _(d):
            s_copy(c, p, d).start()

    def stage_c(c, p):
        @pl.loop(1, nf)
        def _(d):
            s_copy(c, p, d).wait_recv()

        acc = psum[c, p, f].astype(jnp.float32)
        for d in range(1, nf):
            acc = acc + zin[c, p, d].astype(jnp.float32)
        if c:
            fin[c, p] = acc.astype(jnp.bfloat16)
            r_copy(c, p).start()
        else:
            ret[p, pl.ds(pl.multiple_of((me // 2) * cap, 16), cap), :] = acc.astype(jnp.bfloat16)

    for g, (c, p) in enumerate(groups):
        stage_a(c, p)
        stage_b(c, p)
        if g:
            stage_c(*groups[g - 1])
    stage_c(*groups[-1])

    for c in range(pairs):
        for p in range(parts):
            h_copy(c, p).wait_send()

            @pl.loop(1, nf)
            def _(d):
                s_copy(c, p, d).wait_send()

            if c:
                r_copy(c, p).wait_send()
    for k in range(1, nt):
        x_copy(k).wait_send()
        for w in range(2):
            if k // 2 not in corner:
                weight_copy(w, k).wait_send()
        for p in range(parts):
            down_copy(k, p).wait_send()
    p_copy(0).wait_send()

    @pl.loop(1, nf)
    def _(d):
        z_copy(d).wait_send()
        p_copy(d).wait_send()

    for c in range(1, pairs):
        for p in range(parts):
            r_copy(c, p).wait_recv()


def finish(wgu, wd, ret, comb_hi, comb_lo, gate_out, up_out, down_out, mixed_out, mixed, out_sem, mixed_sem):
    nt, parts, _, cc = wd.shape
    cols = parts * cc
    copies = []
    for s in range(nt):
        for w, out in enumerate((gate_out, up_out)):
            to = out.at[0, :, pl.ds(s * cols, cols)]
            copies.append(pltpu.make_async_copy(wgu.at[w, s], to, out_sem.at[w, s, 0]))
        for p in range(parts):
            to = down_out.at[0, :, pl.ds(s * cols + p * cc, cc)]
            copies.append(pltpu.make_async_copy(wd.at[s, p], to, out_sem.at[2, s, p]))
    for copy in copies:
        copy.start()
    for p in range(parts):
        back = ret[p]
        value = dot(comb_hi[...], back, TN) + dot(comb_lo[...], back, TN)
        mixed[:, p * cc : (p + 1) * cc] = value.astype(jnp.bfloat16)
    last = pltpu.make_async_copy(mixed, mixed_out, mixed_sem)
    last.start()
    for copy in copies:
        copy.wait()
    last.wait()


def local(tokens, norm_gain, gate_master, up_master, down_master, routes, route_logits):
    nf, nt = lax.axis_size("fs"), lax.axis_size("tp")
    rows, cols = tokens.shape
    block = gate_master.shape[1]
    half = rows * routes.shape[1] // nt
    cap = 2 * half
    every = nf * cap
    pairs = nt // 2
    parts = cols // 128 if cols % 128 == 0 else 1
    cc = cols // parts
    bf16 = jnp.bfloat16
    hbm = pl.BlockSpec(memory_space=pltpu.HBM)
    vmem = pl.BlockSpec(memory_space=pltpu.VMEM)
    dma = pltpu.SemaphoreType.DMA
    kept = (
        jax.ShapeDtypeStruct((2, nt, block, cols), bf16),
        jax.ShapeDtypeStruct((nt, parts, block, cc), bf16),
        jax.ShapeDtypeStruct((parts, nt * half, cc), bf16),
        jax.ShapeDtypeStruct((nt * half, rows), bf16),
        jax.ShapeDtypeStruct((nt * half, rows), bf16),
    )
    held = pl.pallas_call(
        functools.partial(kernel, nf, nt),
        out_shape=kept,
        in_specs=[hbm] * 7,
        out_specs=(vmem,) * 5,
        scratch_shapes=[
            pltpu.VMEM((rows, cols), bf16),
            pltpu.VMEM((1, cols), jnp.float32),
            pltpu.VMEM((2, rows), jnp.int32),
            pltpu.VMEM((2, rows), jnp.float32),
            pltpu.VMEM((SLOTS, block, cols), jnp.float32),
            pltpu.VMEM((2, nt - 1, block, cols), bf16),
            pltpu.VMEM((nt - 1, parts, block, cc), bf16),
            pltpu.VMEM((nt, half, cols), bf16),
            pltpu.VMEM((nt, half, cols), bf16),
            pltpu.VMEM((nt, every, cols), bf16),
            pltpu.VMEM((every, block), jnp.float32),
            pltpu.VMEM((every, block), bf16),
            pltpu.VMEM((pairs, parts, every, cc), bf16),
            pltpu.VMEM((pairs, parts, every, cc), bf16),
            pltpu.VMEM((pairs, parts, nf, cap, cc), bf16),
            pltpu.VMEM((pairs, parts, nf, cap, cc), bf16),
            pltpu.VMEM((pairs, parts, cap, cc), bf16),
            dma((4,)),
            dma((SLOTS,)),
            dma((2, nt - 1)), dma((2, nt - 1)),
            dma((nt - 1, parts)), dma((nt - 1, parts)),
            dma((nt - 1,)), dma((nt - 1,)),
            dma((nf,)), dma((nf,)),
            dma((nf,)), dma((nf,)),
            dma((pairs, parts)), dma((pairs, parts)),
            dma((pairs, parts, nf)), dma((pairs, parts, nf)),
            dma((pairs, parts)), dma((pairs, parts)),
        ],
        compiler_params=pltpu.CompilerParams(
            collective_id=0, has_side_effects=True, vmem_limit_bytes=40 * 1024 * 1024
        ),
    )(tokens, norm_gain.reshape(1, cols), gate_master, up_master, down_master, routes.T, route_logits.T)
    served = jax.ShapeDtypeStruct((1, block, nt * cols), bf16)
    return pl.pallas_call(
        finish,
        out_shape=(served, served, served, jax.ShapeDtypeStruct((rows, cols), bf16)),
        in_specs=[vmem] * 5,
        out_specs=(hbm,) * 4,
        scratch_shapes=[pltpu.VMEM((rows, cols), bf16), dma((3, nt, parts)), dma(())],
        compiler_params=pltpu.CompilerParams(vmem_limit_bytes=16 * 1024 * 1024),
    )(*held)


def solution(mesh):
    placed = (
        P("fs", "tp"),
        P("tp"),
        P(None, "fs", "tp"),
        P(None, "fs", "tp"),
        P(None, "fs", "tp"),
        P("fs", None),
        P("fs", None),
    )
    return jax.shard_map(
        local,
        mesh=mesh,
        in_specs=placed,
        out_specs=(P("tp", "fs", None), P("tp", "fs", None), P("tp", "fs", None), P("fs", "tp")),
        check_vma=False,
    )
```

```python
import functools

import jax
import jax.numpy as jnp
from jax import lax
from jax.experimental import pallas as pl
from jax.experimental.pallas import tpu as pltpu
from jax.sharding import PartitionSpec as P

epsilon = 1e-05
MESH = pl.DeviceIdType.MESH
NT = (((1,), (1,)), ((), ()))
NN = (((1,), (0,)), ((), ()))
TN = (((0,), (0,)), ((), ()))
SLOTS = 4
EARLY = 2
LAG = 2


def dot(a, b, dims):
    return lax.dot_general(a, b, dims, preferred_element_type=jnp.float32)


def flipped(index, mask):
    result, bit = index, 1
    while bit <= mask:
        if mask & bit:
            result = result + bit * (1 - 2 * ((index // bit) % 2))
        bit *= 2
    return result


def kernel(
    nf, nt, tok_hbm, gain_hbm, gate_ref, up_ref, down_ref, routes_hbm, logits_hbm,
    wgu, wd, ret, comb_hi, comb_lo,
    tok, gain_ref, routes_ref, logits_ref, stage, snd, sdn, pick, xin, xall, gate_pre, hid,
    ship, pin, psum, zin, fin,
    in_sem, stage_sem, w_send, w_recv, d_send, d_recv, x_send, x_recv, z_send, z_recv, p_send, p_recv,
    h_send, h_recv, s_send, s_recv, r_send, r_recv,
):
    f, me = lax.axis_index("fs"), lax.axis_index("tp")
    parity = me % 2
    partner = me + 1 - 2 * parity
    rows, cols = tok.shape
    block = gate_ref.shape[1]
    parts, cc = wd.shape[1], wd.shape[3]
    half = pick.shape[1]
    cap = 2 * half
    experts = nt // 2
    pairs = nt // 2
    masters = (gate_ref, up_ref, down_ref)
    corner = [c for c in range(pairs - 1, 0, -1) if c.bit_count() > 1]
    near = [1] if pairs > 1 else []
    later = [c for c in range(pairs - 1, 1, -1) if c not in corner]

    def both(chips):
        return [k for c in chips for k in (2 * c + 1, 2 * c)]

    order = both(corner + near + later) + [1, 0]
    even, odd = both(corner + near), both(near + corner)

    def peer(k):
        if isinstance(k, tuple):
            a, b = k
            return a + parity * (b - a), flipped(me, a) + parity * (flipped(me, b) - flipped(me, a))
        return k, flipped(me, k)

    crossing = list(zip(even, odd))
    straight = both(later)
    first = []
    for j in range(max(len(crossing), len(straight))):
        first += crossing[j : j + 1] + straight[j : j + 1]
    first += [1, 0]
    last = both(near + later) + [1, 0] + both(corner)
    jobs = [(w, k) for w in range(2) for k in first] + [(2, k) for k in last]

    def load(i):
        w, k = jobs[i]
        return pltpu.make_async_copy(
            masters[w].at[peer(k)[1]], stage.at[i % SLOTS], stage_sem.at[i % SLOTS]
        )

    def remote(src, dst, send, recv, to_f, to_t):
        return pltpu.make_async_remote_copy(
            src_ref=src, dst_ref=dst, send_sem=send, recv_sem=recv,
            device_id=(to_f, to_t), device_id_type=MESH,
        )

    small = [
        pltpu.make_async_copy(a, b, in_sem.at[i])
        for i, (a, b) in enumerate(
            ((gain_hbm, gain_ref), (routes_hbm, routes_ref), (logits_hbm, logits_ref), (tok_hbm, tok))
        )
    ]
    load(0).start()
    for copy in small:
        copy.start()
    for i in range(1, SLOTS):
        load(i).start()
    barrier = pltpu.get_barrier_semaphore()
    for k in range(1, nt):
        pl.semaphore_signal(barrier, inc=1, device_id=(f, flipped(me, k)), device_id_type=MESH)

    @pl.loop(1, nf)
    def _(d):
        pl.semaphore_signal(barrier, inc=1, device_id=((f + d) % nf, me), device_id_type=MESH)

    step = 128 if block % 128 == 0 else block

    def weight_copy(w, k):
        k, to = peer(k)
        return remote(snd.at[w, k - 1], wgu.at[w, me], w_send.at[w, k - 1], w_recv.at[w, k - 1], f, to)

    def down_copy(k, p):
        return remote(
            sdn.at[k - 1, p], wd.at[me, p], d_send.at[k - 1, p], d_recv.at[k - 1, p], f, flipped(me, k)
        )

    def convert(i):
        w, k = jobs[i]
        slot = i % SLOTS
        load(i).wait()
        gain = gain_ref[...]

        @pl.loop(0, block // step)
        def _(c):
            at = pl.ds(pl.multiple_of(c * step, 16), step)
            value = stage[slot, at, :]
            if w < 2:
                value = (value * gain).astype(jnp.bfloat16)
                if k:
                    snd[w, peer(k)[0] - 1, at, :] = value
                else:
                    wgu[w, me, at, :] = value
            else:
                value = value.astype(jnp.bfloat16)
                for p in range(parts):
                    piece = value[:, p * cc : (p + 1) * cc]
                    if k:
                        sdn[k - 1, p, at, :] = piece
                    else:
                        wd[me, p, at, :] = piece

        if i + SLOTS < len(jobs):
            load(i + SLOTS).start()

    def send(i):
        w, k = jobs[i]
        if not k:
            return
        if w < 2:
            weight_copy(w, k).start()
        elif k % 2 == 0:
            for p in range(parts):
                down_copy(k + 1, p).start()
                down_copy(k, p).start()
        elif k == 1:
            for p in range(parts):
                down_copy(k, p).start()

    def x_copy(k):
        to = flipped(me, k)
        return remote(pick.at[to], xin.at[me], x_send.at[k - 1], x_recv.at[k - 1], f, to)

    def route():
        for copy in small[1:]:
            copy.wait()
        r0, r1 = routes_ref[0:1, :], routes_ref[1:2, :]
        l0, l1 = logits_ref[0:1, :], logits_ref[1:2, :]
        p0 = 1.0 / (1.0 + jnp.exp(l1 - l0))
        p1 = 1.0 / (1.0 + jnp.exp(l0 - l1))
        padded = -(-experts // 8) * 8
        ids = lax.broadcasted_iota(jnp.int32, (padded, rows), 0)
        first = jnp.where(ids == r0, 1.0, 0.0)
        second = jnp.where(ids == r1, 1.0, 0.0)
        chosen = first + second
        weight = first * p0 + second * p1
        before = lax.broadcasted_iota(jnp.int32, (rows, rows), 0)
        after = lax.broadcasted_iota(jnp.int32, (rows, rows), 1)
        upto = jnp.where(before <= after, 1.0, 0.0).astype(jnp.bfloat16)
        position = dot(chosen.astype(jnp.bfloat16), upto, NN) - 1.0
        slots = lax.broadcasted_iota(jnp.int32, (cap, rows), 0).astype(jnp.float32)
        for e in range(experts):
            hit = jnp.where(slots == position[e : e + 1, :], 1.0, 0.0) * chosen[e : e + 1, :]
            placed = hit.astype(jnp.bfloat16)
            scaled = hit * weight[e : e + 1, :]
            high = scaled.astype(jnp.bfloat16)
            at = pl.ds(e * cap, cap)
            comb_hi[at, :] = high
            comb_lo[at, :] = (scaled - high.astype(jnp.float32)).astype(jnp.bfloat16)
            got = dot(placed, tok[...], NN).astype(jnp.bfloat16)
            pick[2 * e] = got[:half]
            pick[2 * e + 1] = got[half:]
        xin[me] = pick[me]
        for k in order[:-1]:
            x_copy(k).start()

    small[0].wait()
    for i in range(EARLY):
        convert(i)
    pl.semaphore_wait(barrier, nt - 1 + nf - 1)
    for i in range(EARLY):
        send(i)
    route()
    for i in range(EARLY, len(jobs)):
        convert(i)
        send(i)

    for k in order[:-1]:
        x_copy(k).wait_recv()
    total = jnp.zeros((half, 1), jnp.float32)
    for s in range(nt):
        v = xin[s].astype(jnp.float32)
        total = total + jnp.sum(v * v, axis=-1, keepdims=True)
    scale = lax.rsqrt(total / (nt * cols) + epsilon)

    def rows_of(p, g):
        return pl.ds(pl.multiple_of((2 * g + p) * half, 16), half)

    mine = rows_of(parity, f)
    for s in range(nt):
        xall[s, mine, :] = (xin[s].astype(jnp.float32) * scale).astype(jnp.bfloat16)

    def z_copy(d):
        here = xall.at[:, mine, :]
        return remote(here, here, z_send.at[d], z_recv.at[d], (f + d) % nf, me)

    def p_copy(d):
        here = xall.at[:, rows_of(parity, (f + nf - d) % nf), :]
        return remote(here, here, p_send.at[d], p_recv.at[d], f, partner)

    p_copy(0).start()

    @pl.loop(1, nf)
    def _(d):
        z_copy(d).start()

    @pl.loop(1, nf)
    def _(d):
        here = xall.at[:, rows_of(parity, (f + nf - d) % nf), :]
        remote(here, here, z_send.at[d], z_recv.at[d], (f + d) % nf, me).wait_recv()
        p_copy(d).start()

    @pl.loop(0, nf)
    def _(d):
        here = xall.at[:, rows_of(1 - parity, (f + nf - d) % nf), :]
        remote(here, here, p_send.at[d], p_recv.at[d], f, partner).wait_recv()

    def arrived(w, k):
        if k:
            s = flipped(me, k)
            remote(
                snd.at[w, k - 1], wgu.at[w, s], w_send.at[w, k - 1], w_recv.at[w, k - 1], f, s
            ).wait_recv()

    def product(w, at):
        acc = dot(xall[0], wgu[w, 0, at, :], NT)
        for s in range(1, nt):
            acc = acc + dot(xall[s], wgu[w, s, at, :], NT)
        return acc

    def tile(c):
        return pl.ds(pl.multiple_of(c * step, 16), step)

    def lanes(c):
        return pl.ds(pl.multiple_of(c * step, 128), step) if block % 128 == 0 else slice(None)

    for k in order:
        arrived(0, k)

    @pl.loop(0, block // step)
    def _(c):
        gate_pre[:, lanes(c)] = product(0, tile(c))

    for k in order:
        arrived(1, k)

    @pl.loop(0, block // step)
    def _(c):
        gate = gate_pre[:, lanes(c)]
        hid[:, lanes(c)] = (gate / (1.0 + jnp.exp(-gate)) * product(1, tile(c))).astype(jnp.bfloat16)

    groups = [(0, p) for p in range(parts)]
    groups += [(c, p) for p in range(parts) for c in near + later]
    groups += [(c, p) for p in range(parts) for c in corner]

    def took(k, p):
        s = flipped(me, k)
        if k:
            remote(
                sdn.at[k - 1, p], wd.at[s, p], d_send.at[k - 1, p], d_recv.at[k - 1, p], f, s
            ).wait_recv()
        return dot(hid[...], wd[s, p], NN)

    def h_copy(c, p):
        return remote(ship.at[c, p], pin.at[c, p], h_send.at[c, p], h_recv.at[c, p], f, partner)

    def s_copy(c, p, d):
        to = (f + d) % nf
        return remote(psum.at[c, p, to], zin.at[c, p, d], s_send.at[c, p, d], s_recv.at[c, p, d], to, me)

    def r_copy(c, p):
        return remote(
            fin.at[c, p], ret.at[p, pl.ds(pl.multiple_of((me // 2) * cap, 16), cap), :],
            r_send.at[c, p], r_recv.at[c, p], f, flipped(me, 2 * c),
        )

    def stage_a(c, p):
        ship[c, p] = took(2 * c + 1, p).astype(jnp.bfloat16)
        h_copy(c, p).start()

    def stage_b(c, p):
        own = took(2 * c, p)
        h_copy(c, p).wait_recv()
        total = (own + pin[c, p].astype(jnp.float32)).astype(jnp.bfloat16)
        for j in range(nf):
            psum[c, p, j] = total[j * cap : (j + 1) * cap]

        @pl.loop(1, nf)
        def _(d):
            s_copy(c, p, d).start()

    def stage_c(c, p):
        @pl.loop(1, nf)
        def _(d):
            s_copy(c, p, d).wait_recv()

        acc = psum[c, p, f].astype(jnp.float32)
        for d in range(1, nf):
            acc = acc + zin[c, p, d].astype(jnp.float32)
        if c:
            fin[c, p] = acc.astype(jnp.bfloat16)
            r_copy(c, p).start()
        else:
            ret[p, pl.ds(pl.multiple_of((me // 2) * cap, 16), cap), :] = acc.astype(jnp.bfloat16)

    for g, (c, p) in enumerate(groups):
        stage_a(c, p)
        stage_b(c, p)
        if g >= LAG:
            stage_c(*groups[g - LAG])
    for c, p in groups[-LAG:]:
        stage_c(c, p)

    for c in range(pairs):
        for p in range(parts):
            h_copy(c, p).wait_send()

            @pl.loop(1, nf)
            def _(d):
                s_copy(c, p, d).wait_send()

            if c:
                r_copy(c, p).wait_send()
    for k in range(1, nt):
        x_copy(k).wait_send()
        for w in range(2):
            weight_copy(w, k).wait_send()
        for p in range(parts):
            down_copy(k, p).wait_send()
    p_copy(0).wait_send()

    @pl.loop(1, nf)
    def _(d):
        z_copy(d).wait_send()
        p_copy(d).wait_send()

    for c in range(1, pairs):
        for p in range(parts):
            r_copy(c, p).wait_recv()


def finish(wgu, wd, ret, comb_hi, comb_lo, gate_out, up_out, down_out, mixed_out, mixed, out_sem, mixed_sem):
    nt, parts, _, cc = wd.shape
    cols = parts * cc
    copies = []
    for s in range(nt):
        for w, out in enumerate((gate_out, up_out)):
            to = out.at[0, :, pl.ds(s * cols, cols)]
            copies.append(pltpu.make_async_copy(wgu.at[w, s], to, out_sem.at[w, s, 0]))
        for p in range(parts):
            to = down_out.at[0, :, pl.ds(s * cols + p * cc, cc)]
            copies.append(pltpu.make_async_copy(wd.at[s, p], to, out_sem.at[2, s, p]))
    for copy in copies:
        copy.start()
    for p in range(parts):
        back = ret[p]
        value = dot(comb_hi[...], back, TN) + dot(comb_lo[...], back, TN)
        mixed[:, p * cc : (p + 1) * cc] = value.astype(jnp.bfloat16)
    last = pltpu.make_async_copy(mixed, mixed_out, mixed_sem)
    last.start()
    for copy in copies:
        copy.wait()
    last.wait()


def local(tokens, norm_gain, gate_master, up_master, down_master, routes, route_logits):
    nf, nt = lax.axis_size("fs"), lax.axis_size("tp")
    rows, cols = tokens.shape
    block = gate_master.shape[1]
    half = rows * routes.shape[1] // nt
    cap = 2 * half
    every = nf * cap
    pairs = nt // 2
    parts = cols // 128 if cols % 128 == 0 else 1
    cc = cols // parts
    bf16 = jnp.bfloat16
    hbm = pl.BlockSpec(memory_space=pltpu.HBM)
    vmem = pl.BlockSpec(memory_space=pltpu.VMEM)
    dma = pltpu.SemaphoreType.DMA
    kept = (
        jax.ShapeDtypeStruct((2, nt, block, cols), bf16),
        jax.ShapeDtypeStruct((nt, parts, block, cc), bf16),
        jax.ShapeDtypeStruct((parts, nt * half, cc), bf16),
        jax.ShapeDtypeStruct((nt * half, rows), bf16),
        jax.ShapeDtypeStruct((nt * half, rows), bf16),
    )
    small = (
        pltpu.with_memory_space_constraint(v, pltpu.HBM)
        for v in (tokens, norm_gain.reshape(1, cols), routes.T, route_logits.T)
    )
    tokens, norm_gain, routes, route_logits = small
    held = pl.pallas_call(
        functools.partial(kernel, nf, nt),
        out_shape=kept,
        in_specs=[hbm] * 7,
        out_specs=(vmem,) * 5,
        scratch_shapes=[
            pltpu.VMEM((rows, cols), bf16),
            pltpu.VMEM((1, cols), jnp.float32),
            pltpu.VMEM((2, rows), jnp.int32),
            pltpu.VMEM((2, rows), jnp.float32),
            pltpu.VMEM((SLOTS, block, cols), jnp.float32),
            pltpu.VMEM((2, nt - 1, block, cols), bf16),
            pltpu.VMEM((nt - 1, parts, block, cc), bf16),
            pltpu.VMEM((nt, half, cols), bf16),
            pltpu.VMEM((nt, half, cols), bf16),
            pltpu.VMEM((nt, every, cols), bf16),
            pltpu.VMEM((every, block), jnp.float32),
            pltpu.VMEM((every, block), bf16),
            pltpu.VMEM((pairs, parts, every, cc), bf16),
            pltpu.VMEM((pairs, parts, every, cc), bf16),
            pltpu.VMEM((pairs, parts, nf, cap, cc), bf16),
            pltpu.VMEM((pairs, parts, nf, cap, cc), bf16),
            pltpu.VMEM((pairs, parts, cap, cc), bf16),
            dma((4,)),
            dma((SLOTS,)),
            dma((2, nt - 1)), dma((2, nt - 1)),
            dma((nt - 1, parts)), dma((nt - 1, parts)),
            dma((nt - 1,)), dma((nt - 1,)),
            dma((nf,)), dma((nf,)),
            dma((nf,)), dma((nf,)),
            dma((pairs, parts)), dma((pairs, parts)),
            dma((pairs, parts, nf)), dma((pairs, parts, nf)),
            dma((pairs, parts)), dma((pairs, parts)),
        ],
        compiler_params=pltpu.CompilerParams(
            collective_id=0, has_side_effects=True, vmem_limit_bytes=40 * 1024 * 1024
        ),
    )(tokens, norm_gain, gate_master, up_master, down_master, routes, route_logits)
    served = jax.ShapeDtypeStruct((1, block, nt * cols), bf16)
    return pl.pallas_call(
        finish,
        out_shape=(served, served, served, jax.ShapeDtypeStruct((rows, cols), bf16)),
        in_specs=[vmem] * 5,
        out_specs=(hbm,) * 4,
        scratch_shapes=[pltpu.VMEM((rows, cols), bf16), dma((3, nt, parts)), dma(())],
        compiler_params=pltpu.CompilerParams(vmem_limit_bytes=16 * 1024 * 1024),
    )(*held)


def solution(mesh):
    placed = (
        P("fs", "tp"),
        P("tp"),
        P(None, "fs", "tp"),
        P(None, "fs", "tp"),
        P(None, "fs", "tp"),
        P("fs", None),
        P("fs", None),
    )
    return jax.shard_map(
        local,
        mesh=mesh,
        in_specs=placed,
        out_specs=(P("tp", "fs", None), P("tp", "fs", None), P("tp", "fs", None), P("fs", "tp")),
        check_vma=False,
    )
```

```python
import functools
import math

import jax
import jax.numpy as jnp
from jax import lax
from jax.experimental import pallas as pl
from jax.experimental.pallas import tpu as pltpu
from jax.sharding import PartitionSpec as P

epsilon = 1e-05
MESH = pl.DeviceIdType.MESH
NT = (((1,), (1,)), ((), ()))
NN = (((1,), (0,)), ((), ()))
TN = (((0,), (0,)), ((), ()))
SLOTS = 4
EARLY = 1
ROUTED = 2
LAG = 2
SPARE = 8 * 1024 * 1024


def dot(a, b, dims):
    return lax.dot_general(a, b, dims, preferred_element_type=jnp.float32)


def flipped(index, mask):
    result, bit = index, 1
    while bit <= mask:
        if mask & bit:
            result = result + bit * (1 - 2 * ((index // bit) % 2))
        bit *= 2
    return result


def kernel(
    nf, nt, tok_hbm, gain_hbm, gate_ref, up_ref, down_ref, routes_hbm, logits_hbm,
    wgu, wd, ret, comb_hi, comb_lo,
    tok, gain_ref, routes_ref, logits_ref, stage, snd, sdn, pick, xin, xall, gate_pre, hid,
    ship, pin, psum, zin, fin,
    in_sem, stage_sem, sent, w_recv, d_recv, one_recv, h_recv, s_recv,
):
    w_send, d_send, x_send, z_send, p_send, h_send, s_send, r_send = (sent.at[i] for i in range(8))
    x_recv, z_recv, p_recv, r_recv = (one_recv.at[i] for i in range(4))
    f, me = lax.axis_index("fs"), lax.axis_index("tp")
    parity = me % 2
    partner = me + 1 - 2 * parity
    rows, cols = tok.shape
    block = gate_ref.shape[1]
    parts, cc = wd.shape[1], wd.shape[3]
    half = pick.shape[1]
    cap = 2 * half
    experts = nt // 2
    pairs = nt // 2
    masters = (gate_ref, up_ref, down_ref)
    corner = [c for c in range(pairs - 1, 0, -1) if c.bit_count() > 1]
    near = [1] if pairs > 1 else []
    later = [c for c in range(pairs - 1, 1, -1) if c not in corner]

    def both(chips):
        return [k for c in chips for k in (2 * c + 1, 2 * c)]

    order = both(corner + near + later) + [1, 0]
    even, odd = both(corner + near), both(near + corner)

    def peer(k):
        if isinstance(k, tuple):
            a, b = k
            return a + parity * (b - a), flipped(me, a) + parity * (flipped(me, b) - flipped(me, a))
        return k, flipped(me, k)

    crossing = list(zip(even, odd))
    straight = both(later)
    first = []
    for j in range(max(len(crossing), len(straight))):
        first += crossing[j : j + 1] + straight[j : j + 1]
    first += [1, 0]
    last = both(near + later) + [1, 0] + both(corner)
    jobs = [(w, k) for w in range(2) for k in first] + [(2, k) for k in last]

    def load(i):
        w, k = jobs[i]
        return pltpu.make_async_copy(
            masters[w].at[peer(k)[1]], stage.at[i % SLOTS], stage_sem.at[i % SLOTS]
        )

    def remote(src, dst, send, recv, to_f, to_t):
        return pltpu.make_async_remote_copy(
            src_ref=src, dst_ref=dst, send_sem=send, recv_sem=recv,
            device_id=(to_f, to_t), device_id_type=MESH,
        )

    small = [
        pltpu.make_async_copy(a, b, in_sem.at[i])
        for i, (a, b) in enumerate(
            ((gain_hbm, gain_ref), (routes_hbm, routes_ref), (logits_hbm, logits_ref), (tok_hbm, tok))
        )
    ]
    small[0].start()
    for i in range(SLOTS):
        load(i).start()
        if not i:
            for copy in small[1:]:
                copy.start()
    barrier = pltpu.get_barrier_semaphore()
    for k in range(1, nt):
        pl.semaphore_signal(barrier, inc=1, device_id=(f, flipped(me, k)), device_id_type=MESH)

    @pl.loop(1, nf)
    def _(d):
        pl.semaphore_signal(barrier, inc=1, device_id=((f + d) % nf, me), device_id_type=MESH)

    step = 128 if block % 128 == 0 else block

    def weight_copy(w, k):
        k, to = peer(k)
        return remote(snd.at[w, k - 1], wgu.at[w, me], w_send, w_recv.at[w], f, to)

    def down_copy(k, p):
        return remote(sdn.at[k - 1, p], wd.at[me, p], d_send, d_recv.at[k - 1, p], f, flipped(me, k))

    def convert(i):
        w, k = jobs[i]
        slot = i % SLOTS
        load(i).wait()
        gain = gain_ref[...]

        @pl.loop(0, block // step)
        def _(c):
            at = pl.ds(pl.multiple_of(c * step, 16), step)
            value = stage[slot, at, :]
            if w < 2:
                value = (value * gain).astype(jnp.bfloat16)
                if k:
                    snd[w, peer(k)[0] - 1, at, :] = value
                else:
                    wgu[w, me, at, :] = value
            else:
                value = value.astype(jnp.bfloat16)
                for p in range(parts):
                    piece = value[:, p * cc : (p + 1) * cc]
                    if k:
                        sdn[k - 1, p, at, :] = piece
                    else:
                        wd[me, p, at, :] = piece

        if i + SLOTS < len(jobs):
            load(i + SLOTS).start()

    def send(i):
        w, k = jobs[i]
        if not k:
            return
        if w < 2:
            weight_copy(w, k).start()
        elif k == 1:
            for p in range(parts):
                down_copy(k, p).start()
        elif k % 2 == 0:
            for p in range(parts):
                down_copy(k, p).start()
                down_copy(k + 1, p).start()

    def x_copy(k):
        to = flipped(me, k)
        return remote(pick.at[to], xin.at[me], x_send, x_recv, f, to)

    def route():
        for copy in small[1:]:
            copy.wait()
        r0, r1 = routes_ref[0:1, :], routes_ref[1:2, :]
        l0, l1 = logits_ref[0:1, :], logits_ref[1:2, :]
        p0 = 1.0 / (1.0 + jnp.exp(l1 - l0))
        p1 = 1.0 / (1.0 + jnp.exp(l0 - l1))
        padded = -(-experts // 8) * 8
        ids = lax.broadcasted_iota(jnp.int32, (padded, rows), 0)
        first = jnp.where(ids == r0, 1.0, 0.0)
        second = jnp.where(ids == r1, 1.0, 0.0)
        chosen = first + second
        weight = first * p0 + second * p1
        before = lax.broadcasted_iota(jnp.int32, (rows, rows), 0)
        after = lax.broadcasted_iota(jnp.int32, (rows, rows), 1)
        upto = jnp.where(before <= after, 1.0, 0.0).astype(jnp.bfloat16)
        position = dot(chosen.astype(jnp.bfloat16), upto, NN) - 1.0
        slots = lax.broadcasted_iota(jnp.int32, (cap, rows), 0).astype(jnp.float32)
        for e in range(experts):
            hit = jnp.where(slots == position[e : e + 1, :], 1.0, 0.0) * chosen[e : e + 1, :]
            placed = hit.astype(jnp.bfloat16)
            scaled = hit * weight[e : e + 1, :]
            high = scaled.astype(jnp.bfloat16)
            at = pl.ds(e * cap, cap)
            comb_hi[at, :] = high
            comb_lo[at, :] = (scaled - high.astype(jnp.float32)).astype(jnp.bfloat16)
            got = dot(placed, tok[...], NN).astype(jnp.bfloat16)
            pick[2 * e] = got[:half]
            pick[2 * e + 1] = got[half:]
        xin[me] = pick[me]
        for k in order[:-1]:
            x_copy(k).start()

    small[0].wait()
    for i in range(EARLY):
        convert(i)
    pl.semaphore_wait(barrier, nt - 1 + nf - 1)
    for i in range(EARLY):
        send(i)
    for i in range(EARLY, ROUTED):
        convert(i)
        send(i)
    route()
    for i in range(ROUTED, len(jobs)):
        convert(i)
        send(i)

    def whole(ref, send, recv):
        return remote(ref, ref, send, recv, f, partner)

    others = pl.ds(0, nt - 1)
    whole(xin.at[others], x_send, x_recv).wait_recv()
    total = jnp.zeros((half, 1), jnp.float32)
    for s in range(nt):
        v = xin[s].astype(jnp.float32)
        total = total + jnp.sum(v * v, axis=-1, keepdims=True)
    scale = lax.rsqrt(total / (nt * cols) + epsilon)

    def rows_of(p, g):
        return pl.ds(pl.multiple_of((2 * g + p) * half, 16), half)

    mine = rows_of(parity, f)
    for s in range(nt):
        xall[s, mine, :] = (xin[s].astype(jnp.float32) * scale).astype(jnp.bfloat16)

    def z_copy(d):
        here = xall.at[:, mine, :]
        return remote(here, here, z_send, z_recv, (f + d) % nf, me)

    def p_copy(d):
        here = xall.at[:, rows_of(parity, (f + nf - d) % nf), :]
        return remote(here, here, p_send, p_recv, f, partner)

    p_copy(0).start()

    @pl.loop(1, nf)
    def _(d):
        z_copy(d).start()

    sides = whole(xall.at[:, pl.ds(0, (nf - 1) * half), :], z_send, z_recv)
    across = whole(xall.at[:, pl.ds(0, nf * half), :], p_send, p_recv)
    sides.wait_recv()

    @pl.loop(1, nf)
    def _(d):
        p_copy(d).start()

    across.wait_recv()

    def arrived(w):
        whole(wgu.at[w, others], w_send, w_recv.at[w]).wait_recv()

    def product(w, at):
        acc = dot(xall[0], wgu[w, 0, at, :], NT)
        for s in range(1, nt):
            acc = acc + dot(xall[s], wgu[w, s, at, :], NT)
        return acc

    def tile(c):
        return pl.ds(pl.multiple_of(c * step, 16), step)

    def lanes(c):
        return pl.ds(pl.multiple_of(c * step, 128), step) if block % 128 == 0 else slice(None)

    arrived(0)

    @pl.loop(0, block // step)
    def _(c):
        gate_pre[:, lanes(c)] = product(0, tile(c))

    arrived(1)

    @pl.loop(0, block // step)
    def _(c):
        gate = gate_pre[:, lanes(c)]
        hid[:, lanes(c)] = (gate / (1.0 + jnp.exp(-gate)) * product(1, tile(c))).astype(jnp.bfloat16)

    groups = [(0, p) for p in range(parts)]
    groups += [(c, p) for p in range(parts) for c in near + later]
    groups += [(c, p) for p in range(parts) for c in corner]

    up = f // ((nf + 1) // 2)

    def took(k, p):
        s = flipped(me, k)
        if k:
            whole(wd.at[s, p], d_send, d_recv.at[k - 1, p]).wait_recv()
        return dot(hid[...], wd[s, p], NN)

    def h_copy(c, p):
        return remote(ship.at[c, p], pin.at[c, p], h_send, h_recv.at[c, p], f, partner)

    def s_copy(c, p, d):
        d = up * d + (1 - up) * (nf - d)
        to = (f + d) % nf
        return remote(psum.at[c, p, to], zin.at[c, p, d], s_send, s_recv.at[c, p], to, me)

    def r_copy(c, p):
        there = ret.at[p, pl.ds(pl.multiple_of((me // 2) * cap, 16), cap), :]
        return remote(fin.at[c, p], there, r_send, r_recv, f, flipped(me, 2 * c + 1))

    def stage_a(c, p):
        ship[c, p] = took(2 * c, p).astype(jnp.bfloat16)
        h_copy(c, p).start()

    def stage_b(c, p):
        own = took(2 * c + 1, p)
        h_copy(c, p).wait_recv()
        total = (own + pin[c, p].astype(jnp.float32)).astype(jnp.bfloat16)
        for j in range(nf):
            psum[c, p, j] = total[j * cap : (j + 1) * cap]

        @pl.loop(1, nf)
        def _(d):
            s_copy(c, p, d).start()

    def stage_c(c, p):
        whole(zin.at[c, p, pl.ds(1, nf - 1)], s_send, s_recv.at[c, p]).wait_recv()
        acc = psum[c, p, f].astype(jnp.float32)
        for d in range(1, nf):
            acc = acc + zin[c, p, d].astype(jnp.float32)
        fin[c, p] = acc.astype(jnp.bfloat16)
        r_copy(c, p).start()

    for g, (c, p) in enumerate(groups):
        stage_a(c, p)
        stage_b(c, p)
        if g >= LAG:
            stage_c(*groups[g - LAG])
    for c, p in groups[-LAG:]:
        stage_c(c, p)

    whole(pick.at[others], x_send, x_recv).wait_send()
    whole(snd, w_send, w_recv.at[0]).wait_send()
    whole(sdn, d_send, d_recv.at[0, 0]).wait_send()
    sides.wait_send()
    across.wait_send()
    whole(ship, h_send, h_recv.at[0, 0]).wait_send()
    whole(psum.at[:, :, pl.ds(0, nf - 1)], s_send, s_recv.at[0, 0]).wait_send()
    whole(fin, r_send, r_recv).wait_send()
    whole(ret, r_send, r_recv).wait_recv()


def finish(wgu, wd, ret, comb_hi, comb_lo, gate_out, up_out, down_out, mixed_out, mixed, out_sem):
    nt, parts, _, cc = wd.shape
    cols = parts * cc
    for s in range(nt):
        for w, out in enumerate((gate_out, up_out)):
            to = out.at[0, :, pl.ds(s * cols, cols)]
            pltpu.make_async_copy(wgu.at[w, s], to, out_sem.at[w]).start()
        for p in range(parts):
            to = down_out.at[0, :, pl.ds(s * cols + p * cc, cc)]
            pltpu.make_async_copy(wd.at[s, p], to, out_sem.at[2]).start()
    for p in range(parts):
        back = ret[p]
        value = dot(comb_hi[...], back, TN) + dot(comb_lo[...], back, TN)
        mixed[:, p * cc : (p + 1) * cc] = value.astype(jnp.bfloat16)
    last = pltpu.make_async_copy(mixed, mixed_out, out_sem.at[3])
    last.start()
    for w, out in enumerate((gate_out, up_out, down_out)):
        pltpu.make_async_copy(out, out, out_sem.at[w]).wait()
    last.wait()


def local(tokens, norm_gain, gate_master, up_master, down_master, routes, route_logits):
    nf, nt = lax.axis_size("fs"), lax.axis_size("tp")
    rows, cols = tokens.shape
    block = gate_master.shape[1]
    half = rows * routes.shape[1] // nt
    cap = 2 * half
    every = nf * cap
    pairs = nt // 2
    parts = cols // 128 if cols % 128 == 0 else 1
    cc = cols // parts
    bf16 = jnp.bfloat16
    hbm = pl.BlockSpec(memory_space=pltpu.HBM)
    vmem = pl.BlockSpec(memory_space=pltpu.VMEM)
    dma = pltpu.SemaphoreType.DMA
    kept = (
        jax.ShapeDtypeStruct((2, nt, block, cols), bf16),
        jax.ShapeDtypeStruct((nt, parts, block, cc), bf16),
        jax.ShapeDtypeStruct((parts, nt * half, cc), bf16),
        jax.ShapeDtypeStruct((nt * half, rows), bf16),
        jax.ShapeDtypeStruct((nt * half, rows), bf16),
    )
    operands = (
        tokens, norm_gain.reshape(1, cols), gate_master, up_master, down_master, routes.T, route_logits.T,
    )
    operands = [pltpu.with_memory_space_constraint(v, pltpu.HBM) for v in operands]
    buffers = [
        pltpu.VMEM((rows, cols), bf16),
        pltpu.VMEM((1, cols), jnp.float32),
        pltpu.VMEM((2, rows), jnp.int32),
        pltpu.VMEM((2, rows), jnp.float32),
        pltpu.VMEM((SLOTS, block, cols), jnp.float32),
        pltpu.VMEM((2, nt - 1, block, cols), bf16),
        pltpu.VMEM((nt - 1, parts, block, cc), bf16),
        pltpu.VMEM((nt, half, cols), bf16),
        pltpu.VMEM((nt, half, cols), bf16),
        pltpu.VMEM((nt, every, cols), bf16),
        pltpu.VMEM((every, block), jnp.float32),
        pltpu.VMEM((every, block), bf16),
        pltpu.VMEM((pairs, parts, every, cc), bf16),
        pltpu.VMEM((pairs, parts, every, cc), bf16),
        pltpu.VMEM((pairs, parts, nf, cap, cc), bf16),
        pltpu.VMEM((pairs, parts, nf, cap, cc), bf16),
        pltpu.VMEM((pairs, parts, cap, cc), bf16),
    ]
    grant = sum(math.prod(v.shape) * jnp.dtype(v.dtype).itemsize for v in buffers) + SPARE
    held = pl.pallas_call(
        functools.partial(kernel, nf, nt),
        out_shape=kept,
        in_specs=[hbm] * 7,
        out_specs=(vmem,) * 5,
        scratch_shapes=[
            *buffers,
            dma((4,)),
            dma((SLOTS,)),
            dma((8,)),
            dma((2,)),
            dma((nt - 1, parts)),
            dma((4,)),
            dma((pairs, parts)),
            dma((pairs, parts)),
        ],
        compiler_params=pltpu.CompilerParams(
            collective_id=0, has_side_effects=True, vmem_limit_bytes=grant
        ),
    )(*operands)
    served = jax.ShapeDtypeStruct((1, block, nt * cols), bf16)
    return pl.pallas_call(
        finish,
        out_shape=(served, served, served, jax.ShapeDtypeStruct((rows, cols), bf16)),
        in_specs=[vmem] * 5,
        out_specs=(hbm,) * 4,
        scratch_shapes=[pltpu.VMEM((rows, cols), bf16), dma((4,))],
        compiler_params=pltpu.CompilerParams(vmem_limit_bytes=16 * 1024 * 1024),
    )(*held)


def solution(mesh):
    placed = (
        P("fs", "tp"),
        P("tp"),
        P(None, "fs", "tp"),
        P(None, "fs", "tp"),
        P(None, "fs", "tp"),
        P("fs", None),
        P("fs", None),
    )
    return jax.shard_map(
        local,
        mesh=mesh,
        in_specs=placed,
        out_specs=(P("tp", "fs", None), P("tp", "fs", None), P("tp", "fs", None), P("fs", "tp")),
        check_vma=False,
    )
```
